32 devices in a mesh: fs: 16 (over z, y, x), tp: 2 (over core).
Axes of the slice: x: 2, y: 2, z: 4, core: 2. Of those that a mesh axis runs over, the one named last changes fastest.
Arguments:
- tokens: bfloat16 [6144, 2048], P('fs'), may hold values from -6 to 6
- mixer_norm_gain: float32 [2048], replicated, may hold values from 0.1 to 1.9
- outer_gate_weight: bfloat16 [2048, 2048], P('fs', 'tp'), may hold values from -0.125 to 0.125
- inner_gate_weight: bfloat16 [2048, 2048], P('fs', 'tp'), may hold values from -0.125 to 0.125
- value_projection_weight: bfloat16 [2048, 2048], P('fs', 'tp'), may hold values from -0.125 to 0.125
- filter_taps_weight: float32 [3, 2048], replicated, may hold values from -3 to 3
- mixer_output_weight: bfloat16 [2048, 2048], P('tp', 'fs'), may hold values from -0.125 to 0.125
- feedforward_norm_gain: float32 [2048], replicated, may hold values from 0.1 to 1.9
- up_projection_weight: bfloat16 [2048, 8192], P('fs', 'tp'), may hold values from -0.125 to 0.125
- down_projection_weight: bfloat16 [8192, 2048], P('tp', 'fs'), may hold values from -0.0625 to 0.0625
Outputs:
- layer_out: bfloat16 [6144, 2048], P('fs')
The draws below stay inside these ranges and needn't reach their ends.
All inputs are finite; a program needn't handle non-finite values.
Results may differ from the reference program's by a relative error of at most 0.02.
Values may be sent and summed in bfloat16 or wider, within the bound.
A program may use at most 128 MiB of HBM per device.

```python
import jax
import jax.numpy as jnp
from jax import lax

MODEL_WIDTH = 2048
MIXER_CHANNELS = 2048
FF = 8192
CONV = 3
TOK_DEV = 384
TOKENS = 6144
N_FS = 16
N_TP = 2


def shard_levels(rng, shape, cuts, smallest, largest):
    level = 1.0
    for axis_at, shards_of in cuts:
        steps = jax.random.uniform(jax.random.fold_in(jax.random.fold_in(rng, 6), axis_at), (shards_of,), jnp.float32, smallest / len(cuts), largest / len(cuts))
        level = level * jnp.repeat(jnp.exp(steps), shape[axis_at] // shards_of).reshape((-1,) + (1,) * (len(shape) - 1 - axis_at))
    return level


def gaussian(stream_key, extent, spread, bound, shards=(), held_as=jnp.bfloat16):
    factor_of = shard_levels(stream_key, extent, shards, -0.22, 0.18) if shards else 1.0
    array = jax.random.normal(stream_key, extent, jnp.float32) * spread * factor_of
    return jnp.minimum(jnp.maximum(array, -bound), bound).astype(held_as)


def setup_inputs(seed: int = 0) -> dict:
    arg_keys = jax.random.split(jax.random.key(seed), 11)
    tokens = gaussian(arg_keys[0], (TOKENS, MODEL_WIDTH), 1.0, 6.0, ((0, 16),))
    mixer_norm_gain = jnp.clip(1.0 + 0.18 * jax.random.normal(arg_keys[1], (MODEL_WIDTH,), jnp.float32), 0.1, 1.9)
    outer_gate_weight = gaussian(arg_keys[2], (MODEL_WIDTH, MIXER_CHANNELS), MODEL_WIDTH ** -0.5, 0.125, ((0, 16), (1, 2)))
    inner_gate_weight = gaussian(arg_keys[3], (MODEL_WIDTH, MIXER_CHANNELS), MODEL_WIDTH ** -0.5, 0.125, ((0, 16), (1, 2)))
    value_projection_weight = gaussian(arg_keys[4], (MODEL_WIDTH, MIXER_CHANNELS), MODEL_WIDTH ** -0.5, 0.125, ((0, 16), (1, 2)))
    filter_taps_weight = gaussian(arg_keys[5], (CONV, MIXER_CHANNELS), 0.577, 3.0, (), jnp.float32)
    mixer_output_weight = gaussian(arg_keys[6], (MIXER_CHANNELS, MODEL_WIDTH), MIXER_CHANNELS ** -0.5, 0.125, ((0, 2), (1, 16)))
    feedforward_norm_gain = jnp.clip(1.0 + 0.18 * jax.random.normal(arg_keys[7], (MODEL_WIDTH,), jnp.float32), 0.1, 1.9)
    up_projection_weight = gaussian(arg_keys[8], (MODEL_WIDTH, FF), MODEL_WIDTH ** -0.5, 0.125, ((0, 16), (1, 2)))
    down_projection_weight = gaussian(arg_keys[9], (FF, MODEL_WIDTH), FF ** -0.5, 0.0625, ((0, 2), (1, 16)))
    return {"tokens": tokens, "mixer_norm_gain": mixer_norm_gain, "outer_gate_weight": outer_gate_weight, "inner_gate_weight": inner_gate_weight, "value_projection_weight": value_projection_weight, "filter_taps_weight": filter_taps_weight, "mixer_output_weight": mixer_output_weight, "feedforward_norm_gain": feedforward_norm_gain, "up_projection_weight": up_projection_weight, "down_projection_weight": down_projection_weight}


def rms_norm(rows, gain):
    floats = rows.astype(jnp.float32)
    scale = lax.rsqrt(lax.optimization_barrier(jnp.mean(floats * floats, axis=-1, keepdims=True)) + 1e-06)
    return (floats * scale * gain).astype(jnp.bfloat16)

def causal_mix(inner_product_rows, taps):
    length = inner_product_rows.shape[0]
    width = taps.shape[0]
    padded = jnp.pad(inner_product_rows, ((width - 1, 0), (0, 0)))
    total = jnp.zeros_like(inner_product_rows)
    for offset in range(width):
        total = total + taps[offset] * padded[offset:offset + length]
    return total

def grouped_sum(left, right, groups):
    count = left.shape[0]
    part = left.shape[1] // groups
    lhs = left.reshape(count, groups, part).astype(jnp.float32)
    rhs = right.reshape(groups, part, right.shape[1]).astype(jnp.float32)
    partial_value = jnp.einsum('rgk,gkd->grd', lhs, rhs).astype(jnp.bfloat16)
    partial_value = lax.optimization_barrier(partial_value).astype(jnp.float32)
    return lax.optimization_barrier(jnp.sum(partial_value, axis=0))

def reference(tokens, mixer_norm_gain, outer_gate_weight, inner_gate_weight, value_projection_weight, filter_taps_weight, mixer_output_weight, feedforward_norm_gain, up_projection_weight, down_projection_weight):

    def one_sequence(rows):
        first_normed_rows = rms_norm(rows, mixer_norm_gain)
        outer_gate_rows = jnp.dot(first_normed_rows, outer_gate_weight, preferred_element_type=jnp.float32).astype(jnp.bfloat16)
        inner_gate_rows = jnp.dot(first_normed_rows, inner_gate_weight, preferred_element_type=jnp.float32).astype(jnp.bfloat16)
        value_rows = jnp.dot(first_normed_rows, value_projection_weight, preferred_element_type=jnp.float32).astype(jnp.bfloat16)
        inner_product_rows = inner_gate_rows.astype(jnp.float32) * value_rows.astype(jnp.float32)
        mixed = (outer_gate_rows.astype(jnp.float32) * causal_mix(inner_product_rows, filter_taps_weight)).astype(jnp.bfloat16)
        resid = (rows.astype(jnp.float32) + grouped_sum(mixed, mixer_output_weight, N_TP)).astype(jnp.bfloat16)
        second = rms_norm(resid, feedforward_norm_gain)
        lifted = jnp.maximum(jnp.dot(second, up_projection_weight, preferred_element_type=jnp.float32), 0.0)
        hidden = (lifted * lifted).astype(jnp.bfloat16)
        return (resid.astype(jnp.float32) + grouped_sum(hidden, down_projection_weight, N_TP)).astype(jnp.bfloat16)
    blocks = tokens.reshape(N_FS, TOK_DEV, MODEL_WIDTH)
    return lax.map(one_sequence, blocks).reshape(TOKENS, MODEL_WIDTH)
```

```python
import functools

import jax
import jax.numpy as jnp
from jax import lax
from jax.experimental import pallas as pl
from jax.experimental.pallas import tpu as pltpu
from jax.sharding import PartitionSpec as P


def rms_norm(rows, gain):
    floats = rows.astype(jnp.float32)
    scale = lax.rsqrt(jnp.mean(floats * floats, axis=-1, keepdims=True) + 1e-06)
    return (floats * scale * gain).astype(jnp.bfloat16)


def causal_mix(inner_product_rows, taps):
    length = inner_product_rows.shape[0]
    width = taps.shape[0]
    padded = jnp.pad(inner_product_rows, ((width - 1, 0), (0, 0)))
    total = jnp.zeros_like(inner_product_rows)
    for offset in range(width):
        total = total + taps[offset] * padded[offset : offset + length]
    return total


def settle(partial_value):
    rounded = lax.optimization_barrier(partial_value.astype(jnp.bfloat16))
    return rounded.astype(jnp.float32)


def on_device(
    tokens,
    mixer_norm_gain,
    outer_gate_weight,
    inner_gate_weight,
    value_projection_weight,
    filter_taps_weight,
    mixer_output_weight,
    feedforward_norm_gain,
    up_projection_weight,
    down_projection_weight,
):
    index = lax.axis_index("tp")
    local_width = outer_gate_weight.shape[1]
    first_normed_rows = rms_norm(tokens, mixer_norm_gain)
    pieces = (
        lax.all_gather(outer_gate_weight, "fs", axis=0, tiled=True),
        lax.all_gather(inner_gate_weight, "fs", axis=0, tiled=True),
        lax.all_gather(value_projection_weight, "fs", axis=0, tiled=True),
    )
    columns = first_normed_rows
    outer_gate_rows, inner_gate_rows, value_rows = tuple(
        (jnp.dot(columns, piece, preferred_element_type=jnp.float32) for piece in pieces)
    )
    outer_gate_rows = outer_gate_rows.astype(jnp.bfloat16)
    inner_gate_rows = inner_gate_rows.astype(jnp.bfloat16)
    value_rows = value_rows.astype(jnp.bfloat16)
    taps = lax.dynamic_slice_in_dim(filter_taps_weight, index * local_width, local_width, 1)
    inner_product_rows = inner_gate_rows.astype(jnp.float32) * value_rows.astype(jnp.float32)
    mixed = (outer_gate_rows.astype(jnp.float32) * causal_mix(inner_product_rows, taps)).astype(
        jnp.bfloat16
    )
    partial_value = settle(
        jnp.dot(
            mixed,
            lax.all_gather(mixer_output_weight, "fs", axis=1, tiled=True),
            preferred_element_type=jnp.float32,
        )
    )
    total = lax.psum(partial_value.astype(jnp.bfloat16), "tp").astype(jnp.float32)
    resid = (tokens.astype(jnp.float32) + total).astype(jnp.bfloat16)
    second = rms_norm(resid, feedforward_norm_gain)
    columns = second
    lifted = jnp.maximum(
        jnp.dot(
            columns,
            lax.all_gather(up_projection_weight, "fs", axis=0, tiled=True),
            preferred_element_type=jnp.float32,
        ),
        0.0,
    )
    hidden = (lifted * lifted).astype(jnp.bfloat16)
    down = jnp.dot(
        hidden,
        lax.all_gather(down_projection_weight, "fs", axis=1, tiled=True),
        preferred_element_type=jnp.float32,
    )
    total_down = lax.psum(settle(down).astype(jnp.bfloat16), "tp").astype(jnp.float32)
    return (resid.astype(jnp.float32) + total_down).astype(jnp.bfloat16)


MESH = pl.DeviceIdType.MESH
CAST = 4
STRIP = 64


def fused_kernel(
    planes,
    tokens,
    gain_one,
    w_outer,
    w_inner,
    w_value,
    taps,
    w_mix,
    gain_two,
    w_up,
    w_down,
    out,
    proj,
    mix,
    up,
    down,
    gathered,
    normed,
    hidden,
    part,
    pair_one,
    pair_two,
    cross_one,
    cross_two,
    resid,
    swap_send,
    swap_recv,
    chain_send,
    chain_recv,
    tok_send,
    tok_recv,
    fwd_send,
    fwd_recv,
    sec_send,
    sec_recv,
    secf_send,
    secf_recv,
    pair_send,
    pair_recv,
    cross_send,
    cross_recv,
    last_send,
    last_recv,
):
    f = lax.axis_index("fs")
    t = lax.axis_index("tp")
    g = f // CAST
    j = lax.rem(f, CAST)
    rows = tokens.shape[0]
    half = rows // 2
    depth = w_outer.shape[0]
    wide = w_outer.shape[1] // CAST
    tall = w_up.shape[1] // CAST
    width = tokens.shape[1]
    mine = pl.multiple_of(t * half, half)
    other = pl.multiple_of((1 - t) * half, half)

    def peer(i):
        return lax.rem(j + i, CAST)

    def at(plane, k, core):
        return {"fs": plane * CAST + k, "tp": core}

    partner = at(g, j, 1 - t)

    def remote(src, dst, send, recv, device):
        return pltpu.make_async_remote_copy(
            src_ref=src,
            dst_ref=dst,
            send_sem=send,
            recv_sem=recv,
            device_id=device,
            device_id_type=MESH,
        )

    barrier = pltpu.get_barrier_semaphore()
    for i in range(1, CAST):
        pl.semaphore_signal(barrier, inc=1, device_id=at(g, peer(i), t), device_id_type=MESH)
    pl.semaphore_signal(barrier, inc=1, device_id=partner, device_id_type=MESH)

    @pl.when(g > 0)
    def _():
        pl.semaphore_signal(barrier, inc=1, device_id=at(g - 1, j, t), device_id_type=MESH)

    @pl.when(g < planes - 1)
    def _():
        pl.semaphore_signal(barrier, inc=1, device_id=at(g + 1, j, t), device_id_type=MESH)

    ends = jnp.minimum(g, 1) + jnp.minimum(planes - 1 - g, 1)
    pl.semaphore_wait(barrier, CAST + ends)

    def lanes(start, size):
        return pl.ds(pl.multiple_of(start, 128), size)

    shards = (w_outer, w_inner, w_value, w_mix, w_up, w_down)

    def block(kind, k):
        if kind < 3:
            return shards[kind].at[:, lanes(k * wide, wide)]
        if kind == 3:
            return w_mix.at[pl.ds(pl.multiple_of(k * wide, wide), wide), :]
        if kind == 4:
            return w_up.at[:, lanes(k * tall, tall)]
        return w_down.at[pl.ds(pl.multiple_of(k * tall, tall), tall), :]

    def place(kind, owner):
        start = pl.multiple_of(owner * depth, depth)
        if kind < 3:
            return proj.at[pl.ds(start, depth), pl.ds(kind * wide, wide)]
        if kind == 3:
            return mix.at[:, lanes(owner * depth, depth)]
        if kind == 4:
            return up.at[pl.ds(start, depth), :]
        return down.at[:, lanes(owner * depth, depth)]

    def swap(kind, i):
        k = peer(i)
        return remote(
            block(kind, k),
            place(kind, f),
            swap_send.at[kind, i],
            swap_recv.at[kind, j],
            at(g, k, t),
        )

    def swap_local(kind):
        return pltpu.make_async_copy(block(kind, j), place(kind, f), swap_recv.at[kind, j])

    def start_swap(kind):
        for i in range(1, CAST):
            swap(kind, i).start()
        swap_local(kind).start()

    def wait_swap(kind, k):
        pltpu.make_async_copy(
            place(kind, g * CAST + k), place(kind, g * CAST + k), swap_recv.at[kind, k]
        ).wait()

    chunks = [(kind, None) for kind in range(4)]
    chunks += [(4, q) for q in range(CAST)] + [(5, q) for q in range(CAST)]

    def slab(w, plane):
        kind, q = chunks[w]
        if q is not None:
            return place(kind, plane * CAST + q)
        start = pl.multiple_of(plane * CAST * depth, CAST * depth)
        if kind < 3:
            return proj.at[pl.ds(start, CAST * depth), pl.ds(kind * wide, wide)]
        return mix.at[:, lanes(plane * CAST * depth, CAST * depth)]

    def hop(w, plane, up_way):
        return remote(
            slab(w, plane),
            slab(w, plane),
            chain_send.at[w, plane, 1 if up_way else 0],
            chain_recv.at[w, plane],
            at(g + 1 if up_way else g - 1, j, t),
        )

    def pump(step):
        for dist in range(planes):
            w = step - dist
            if w < 0 or w >= len(chunks):
                continue
            if dist == 0:
                kind, q = chunks[w]
                for k in range(CAST) if q is None else (q,):
                    wait_swap(kind, k)

                @pl.when(g < planes - 1)
                def _():
                    hop(w, g, True).start()

                @pl.when(g > 0)
                def _():
                    hop(w, g, False).start()

            else:

                @pl.when(g - dist >= 0)
                def _():
                    source = g - dist
                    pltpu.make_async_copy(
                        slab(w, source), slab(w, source), chain_recv.at[w, source]
                    ).wait()

                    @pl.when(g < planes - 1)
                    def _():
                        hop(w, source, True).start()

                @pl.when(g + dist < planes)
                def _():
                    source = g + dist
                    pltpu.make_async_copy(
                        slab(w, source), slab(w, source), chain_recv.at[w, source]
                    ).wait()

                    @pl.when(g > 0)
                    def _():
                        hop(w, source, False).start()

    def drain():
        for kind in range(6):
            for i in range(1, CAST):
                swap(kind, i).wait_send()
        for w in range(len(chunks)):
            for plane in range(planes):

                @pl.when(jnp.logical_and(g >= plane, g < planes - 1))
                def _():
                    hop(w, plane, True).wait_send()

                @pl.when(jnp.logical_and(g <= plane, g > 0))
                def _():
                    hop(w, plane, False).wait_send()

    def spread(source, i, send, recv):
        return remote(
            source, gathered.at[j, pl.ds(mine, half)], send.at[i], recv.at[i], at(g, peer(i), t)
        )

    def landed(i):
        return gathered.at[lax.rem(j + CAST - i, CAST), pl.ds(mine, half)]

    def relay(i, send, recv):
        return remote(landed(i), landed(i), send.at[i], recv.at[i], partner)

    def relayed(i, recv):
        ref = gathered.at[lax.rem(j + CAST - i, CAST), pl.ds(other, half)]
        return pltpu.make_async_copy(ref, ref, recv.at[i])

    def arrived(i, recv):
        return pltpu.make_async_copy(landed(i), landed(i), recv.at[i])

    def norm(x, gain):
        floats = x.astype(jnp.float32)
        scale = lax.rsqrt(jnp.mean(floats * floats, axis=-1, keepdims=True) + 1e-06)
        return (floats * scale * gain).astype(jnp.bfloat16)

    own = tokens.at[pl.ds(mine, half)]
    for kind in range(4):
        start_swap(kind)
    for i in range(1, CAST):
        spread(own, i, tok_send, tok_recv).start()
    for kind in (4, 5):
        start_swap(kind)
    keep = pltpu.make_async_copy(tokens, gathered.at[j], tok_recv.at[0])
    keep.start()

    for step in range(3):
        pump(step)
    for i in range(1, CAST):
        arrived(i, tok_recv).wait()
        relay(i, fwd_send, fwd_recv).start()
    pump(3)
    for i in range(1, CAST):
        spread(own, i, tok_send, tok_recv).wait_send()
        relay(i, fwd_send, fwd_recv).wait_send()
        relayed(i, fwd_recv).wait()
    keep.wait()
    for step in range(4, 4 + planes - 1):
        pump(step)
    done = 4 + planes - 1
    total = len(chunks) + planes - 1

    channel = lanes((t * CAST + j) * wide, wide)
    dims = (((1,), (0,)), ((), ()))

    def dot(a, b):
        return lax.dot_general(a, b, dims, preferred_element_type=jnp.float32)

    def mixer(s):
        @pl.loop(0, rows // STRIP)
        def _(r):
            at_rows = pl.ds(pl.multiple_of(r * STRIP, STRIP), STRIP)
            normed[at_rows, :] = norm(gathered[s, at_rows, :], gain_one[...])

        x = normed[...]
        outer = dot(x, proj[:, 0:wide]).astype(jnp.bfloat16).astype(jnp.float32)
        carrier = dot(x, proj[:, wide : 2 * wide]).astype(jnp.bfloat16).astype(jnp.float32)
        values = dot(x, proj[:, 2 * wide : 3 * wide]).astype(jnp.bfloat16).astype(jnp.float32)
        inner = carrier * values
        count = taps.shape[0]
        position = lax.broadcasted_iota(jnp.int32, inner.shape, 0)
        conv = taps[count - 1 : count, channel] * inner
        for back in range(1, count):
            moved = jnp.where(position >= back, pltpu.roll(inner, back, 0), 0.0)
            conv = conv + taps[count - 1 - back : count - back, channel] * moved
        mixed = (outer * conv).astype(jnp.bfloat16)
        for n in range(0, width, 512):
            part[s, :, n : n + 512] = dot(mixed, mix[:, n : n + 512]).astype(jnp.bfloat16)

    def feed_up(s):
        for n in range(0, tall, 256):
            lifted = jnp.maximum(dot(gathered[s], up[:, n : n + 256]), 0.0)
            hidden[s, :, n : n + 256] = (lifted * lifted).astype(jnp.bfloat16)

    def feed_down(s):
        for n in range(0, width, 256):
            part[s, :, n : n + 256] = dot(hidden[s], down[:, n : n + 256]).astype(jnp.bfloat16)

    def pair(turn, i, buffer):
        s = peer(i)
        return remote(
            part.at[s, pl.ds(other, half)],
            buffer.at[s],
            pair_send.at[turn, i],
            pair_recv.at[turn, i],
            partner,
        )

    def pair_wait(turn, i, buffer):
        s = peer(i)
        pltpu.make_async_copy(buffer.at[s], buffer.at[s], pair_recv.at[turn, i]).wait()

    def cross(turn, i, buffer, target):
        return remote(
            buffer.at[peer(i)],
            target.at[i - 1],
            cross_send.at[turn, i],
            cross_recv.at[turn, i],
            at(g, peer(i), t),
        )

    def cross_wait(turn, i, target):
        ref = target.at[i - 1]
        pltpu.make_async_copy(ref, ref, cross_recv.at[turn, i]).wait()

    def strip(r, start=0):
        return pl.ds(pl.multiple_of(start + r * STRIP, STRIP), STRIP)

    def add_pair(i, buffer):
        s = peer(i)

        @pl.loop(0, half // STRIP)
        def _(r):
            a = part[s, strip(r, mine), :].astype(jnp.float32)
            buffer[s, strip(r), :] = (a + buffer[s, strip(r), :].astype(jnp.float32)).astype(
                jnp.bfloat16
            )

    def add_cross(r, buffer, target):
        value = buffer[j, strip(r), :].astype(jnp.float32)
        for i in range(CAST - 1):
            value = value + target[i, strip(r), :].astype(jnp.float32)
        return value

    order = list(range(1, CAST)) + [0]
    for i in order:
        mixer(peer(i))
        pair(0, i, pair_one).start()
        if i == 2:
            pump(done)
    pump(done + 1)
    for i in order:
        pair_wait(0, i, pair_one)
        add_pair(i, pair_one)
        if i:
            cross(0, i, pair_one, cross_one).start()
    pump(done + 2)
    for i in range(1, CAST):
        cross_wait(0, i, cross_one)

    @pl.loop(0, half // STRIP)
    def _(r):
        total_mix = add_cross(r, pair_one, cross_one)
        row = tokens[strip(r, mine), :].astype(jnp.float32) + total_mix
        row = row.astype(jnp.bfloat16)
        resid[strip(r), :] = row
        gathered[j, strip(r, mine), :] = norm(row, gain_two[...])

    fresh = gathered.at[j, pl.ds(mine, half)]
    for i in range(1, CAST):
        spread(fresh, i, sec_send, sec_recv).start()
    relay(0, secf_send, secf_recv).start()
    for i in order:
        pair(0, i, pair_one).wait_send()
        if i:
            cross(0, i, pair_one, cross_one).wait_send()
    pump(done + 3)
    for i in range(1, CAST):
        arrived(i, sec_recv).wait()
        relay(i, secf_send, secf_recv).start()
    pump(done + 4)
    for i in order:
        relayed(i, secf_recv).wait()
    for i in order:
        feed_up(peer(i))
    for step in range(done + 5, total):
        pump(step)
    for i in order:
        feed_down(peer(i))
        pair(1, i, pair_two).start()
    for i in order:
        pair_wait(1, i, pair_two)
        add_pair(i, pair_two)
        if i:
            cross(1, i, pair_two, cross_two).start()
    drain()
    for i in range(1, CAST):
        spread(fresh, i, sec_send, sec_recv).wait_send()
    for i in order:
        relay(i, secf_send, secf_recv).wait_send()
    for i in range(1, CAST):
        cross_wait(1, i, cross_two)

    @pl.loop(0, half // STRIP)
    def _(r):
        value = resid[strip(r), :].astype(jnp.float32) + add_cross(r, pair_two, cross_two)
        out[strip(r, mine), :] = value.astype(jnp.bfloat16)

    final = remote(
        out.at[pl.ds(mine, half)],
        out.at[pl.ds(mine, half)],
        last_send.at[0],
        last_recv.at[0],
        partner,
    )
    final.start()
    for i in order:
        pair(1, i, pair_two).wait_send()
        if i:
            cross(1, i, pair_two, cross_two).wait_send()
    final.wait()


def fused(
    tokens,
    mixer_norm_gain,
    outer_gate_weight,
    inner_gate_weight,
    value_projection_weight,
    filter_taps_weight,
    mixer_output_weight,
    feedforward_norm_gain,
    up_projection_weight,
    down_projection_weight,
):
    rows, width = tokens.shape
    half = rows // 2
    planes = width // (outer_gate_weight.shape[0] * CAST)
    wide = outer_gate_weight.shape[1] // CAST
    tall = up_projection_weight.shape[1] // CAST
    dma = pltpu.SemaphoreType.DMA
    chunk_count = 4 + 2 * CAST
    bf16 = jnp.bfloat16
    return pl.pallas_call(
        functools.partial(fused_kernel, planes),
        out_shape=jax.ShapeDtypeStruct((rows, width), bf16),
        in_specs=[pl.BlockSpec(memory_space=pltpu.VMEM)] * 10,
        out_specs=pl.BlockSpec(memory_space=pltpu.VMEM),
        scratch_shapes=[
            pltpu.VMEM((width, 3 * wide), bf16),
            pltpu.VMEM((wide, width), bf16),
            pltpu.VMEM((width, tall), bf16),
            pltpu.VMEM((tall, width), bf16),
            pltpu.VMEM((CAST, rows, width), bf16),
            pltpu.VMEM((rows, width), bf16),
            pltpu.VMEM((CAST, rows, tall), bf16),
            pltpu.VMEM((CAST, rows, width), bf16),
            pltpu.VMEM((CAST, half, width), bf16),
            pltpu.VMEM((CAST, half, width), bf16),
            pltpu.VMEM((CAST - 1, half, width), bf16),
            pltpu.VMEM((CAST - 1, half, width), bf16),
            pltpu.VMEM((half, width), bf16),
            dma((6, CAST)),
            dma((6, CAST)),
            dma((chunk_count, planes, 2)),
            dma((chunk_count, planes)),
            dma((CAST,)),
            dma((CAST,)),
            dma((CAST,)),
            dma((CAST,)),
            dma((CAST,)),
            dma((CAST,)),
            dma((CAST,)),
            dma((CAST,)),
            dma((2, CAST)),
            dma((2, CAST)),
            dma((2, CAST)),
            dma((2, CAST)),
            dma((1,)),
            dma((1,)),
        ],
        compiler_params=pltpu.CompilerParams(
            collective_id=1, has_side_effects=True, vmem_limit_bytes=63 * 1024 * 1024
        ),
        name="fused_layer",
    )(
        tokens,
        mixer_norm_gain.reshape(1, -1),
        outer_gate_weight,
        inner_gate_weight,
        value_projection_weight,
        filter_taps_weight,
        mixer_output_weight,
        feedforward_norm_gain.reshape(1, -1),
        up_projection_weight,
        down_projection_weight,
    )


def layer(*args):
    tokens, outer, up = args[0], args[2], args[8]
    depth = outer.shape[0]
    fits = (
        lax.axis_size("tp") == 2
        and lax.axis_size("fs") % CAST == 0
        and depth % 128 == 0
        and outer.shape[1] % (CAST * 128) == 0
        and up.shape[1] % (CAST * 256) == 0
        and tokens.shape[0] % (2 * STRIP) == 0
        and tokens.shape[1] % 512 == 0
    )
    return fused(*args) if fits else on_device(*args)


def solution(mesh):
    return jax.shard_map(
        layer,
        mesh=mesh,
        in_specs=(
            P("fs", None),
            P(),
            P("fs", "tp"),
            P("fs", "tp"),
            P("fs", "tp"),
            P(),
            P("tp", "fs"),
            P(),
            P("fs", "tp"),
            P("tp", "fs"),
        ),
        out_specs=P("fs", None),
        check_vma=False,
    )
```

```python
import functools

import jax
import jax.numpy as jnp
from jax import lax
from jax.experimental import pallas as pl
from jax.experimental.pallas import tpu as pltpu
from jax.sharding import PartitionSpec as P


def rms_norm(rows, gain):
    floats = rows.astype(jnp.float32)
    scale = lax.rsqrt(jnp.mean(floats * floats, axis=-1, keepdims=True) + 1e-06)
    return (floats * scale * gain).astype(jnp.bfloat16)


def causal_mix(inner_product_rows, taps):
    length = inner_product_rows.shape[0]
    width = taps.shape[0]
    padded = jnp.pad(inner_product_rows, ((width - 1, 0), (0, 0)))
    total = jnp.zeros_like(inner_product_rows)
    for offset in range(width):
        total = total + taps[offset] * padded[offset : offset + length]
    return total


def settle(partial_value):
    rounded = lax.optimization_barrier(partial_value.astype(jnp.bfloat16))
    return rounded.astype(jnp.float32)


def on_device(
    tokens,
    mixer_norm_gain,
    outer_gate_weight,
    inner_gate_weight,
    value_projection_weight,
    filter_taps_weight,
    mixer_output_weight,
    feedforward_norm_gain,
    up_projection_weight,
    down_projection_weight,
):
    index = lax.axis_index("tp")
    local_width = outer_gate_weight.shape[1]
    first_normed_rows = rms_norm(tokens, mixer_norm_gain)
    pieces = (
        lax.all_gather(outer_gate_weight, "fs", axis=0, tiled=True),
        lax.all_gather(inner_gate_weight, "fs", axis=0, tiled=True),
        lax.all_gather(value_projection_weight, "fs", axis=0, tiled=True),
    )
    columns = first_normed_rows
    outer_gate_rows, inner_gate_rows, value_rows = tuple(
        (jnp.dot(columns, piece, preferred_element_type=jnp.float32) for piece in pieces)
    )
    outer_gate_rows = outer_gate_rows.astype(jnp.bfloat16)
    inner_gate_rows = inner_gate_rows.astype(jnp.bfloat16)
    value_rows = value_rows.astype(jnp.bfloat16)
    taps = lax.dynamic_slice_in_dim(filter_taps_weight, index * local_width, local_width, 1)
    inner_product_rows = inner_gate_rows.astype(jnp.float32) * value_rows.astype(jnp.float32)
    mixed = (outer_gate_rows.astype(jnp.float32) * causal_mix(inner_product_rows, taps)).astype(
        jnp.bfloat16
    )
    partial_value = settle(
        jnp.dot(
            mixed,
            lax.all_gather(mixer_output_weight, "fs", axis=1, tiled=True),
            preferred_element_type=jnp.float32,
        )
    )
    total = lax.psum(partial_value.astype(jnp.bfloat16), "tp").astype(jnp.float32)
    resid = (tokens.astype(jnp.float32) + total).astype(jnp.bfloat16)
    second = rms_norm(resid, feedforward_norm_gain)
    columns = second
    lifted = jnp.maximum(
        jnp.dot(
            columns,
            lax.all_gather(up_projection_weight, "fs", axis=0, tiled=True),
            preferred_element_type=jnp.float32,
        ),
        0.0,
    )
    hidden = (lifted * lifted).astype(jnp.bfloat16)
    down = jnp.dot(
        hidden,
        lax.all_gather(down_projection_weight, "fs", axis=1, tiled=True),
        preferred_element_type=jnp.float32,
    )
    total_down = lax.psum(settle(down).astype(jnp.bfloat16), "tp").astype(jnp.float32)
    return (resid.astype(jnp.float32) + total_down).astype(jnp.bfloat16)


MESH = pl.DeviceIdType.MESH
CAST = 4
STRIP = 64


def fused_kernel(
    planes,
    tokens,
    gain_one,
    w_outer,
    w_inner,
    w_value,
    taps,
    w_mix,
    gain_two,
    w_up,
    w_down,
    out,
    proj,
    mix,
    up,
    down,
    gathered,
    normed,
    hidden,
    part,
    pair_one,
    pair_two,
    cross_one,
    cross_two,
    resid,
    swap_send,
    swap_recv,
    chain_send,
    chain_recv,
    tok_send,
    tok_recv,
    fwd_send,
    fwd_recv,
    sec_send,
    sec_recv,
    secf_send,
    secf_recv,
    pair_send,
    pair_recv,
    cross_send,
    cross_recv,
    set_send,
    set_recv,
    last_send,
    last_recv,
):
    f = lax.axis_index("fs")
    t = lax.axis_index("tp")
    g = f // CAST
    j = lax.rem(f, CAST)
    rows = tokens.shape[0]
    half = rows // 2
    depth = w_outer.shape[0]
    wide = w_outer.shape[1] // CAST
    tall = w_up.shape[1] // CAST
    width = tokens.shape[1]
    mine = pl.multiple_of(t * half, half)
    other = pl.multiple_of((1 - t) * half, half)

    def peer(i):
        return lax.rem(j + i, CAST)

    def at(plane, k, core):
        return {"fs": plane * CAST + k, "tp": core}

    partner = at(g, j, 1 - t)

    def remote(src, dst, send, recv, device):
        return pltpu.make_async_remote_copy(
            src_ref=src,
            dst_ref=dst,
            send_sem=send,
            recv_sem=recv,
            device_id=device,
            device_id_type=MESH,
        )

    barrier = pltpu.get_barrier_semaphore()
    for i in range(1, CAST):
        pl.semaphore_signal(barrier, inc=1, device_id=at(g, peer(i), t), device_id_type=MESH)
    pl.semaphore_signal(barrier, inc=1, device_id=partner, device_id_type=MESH)

    @pl.when(g > 0)
    def _():
        pl.semaphore_signal(barrier, inc=1, device_id=at(g - 1, j, t), device_id_type=MESH)

    @pl.when(g < planes - 1)
    def _():
        pl.semaphore_signal(barrier, inc=1, device_id=at(g + 1, j, t), device_id_type=MESH)

    ends = jnp.minimum(g, 1) + jnp.minimum(planes - 1 - g, 1)
    pl.semaphore_wait(barrier, CAST + ends)

    def lanes(start, size):
        return pl.ds(pl.multiple_of(start, 128), size)

    shards = (w_outer, w_inner, w_value, w_mix, w_up, w_down)

    def block(kind, k):
        if kind < 3:
            return shards[kind].at[:, lanes(k * wide, wide)]
        if kind == 3:
            return w_mix.at[pl.ds(pl.multiple_of(k * wide, wide), wide), :]
        if kind == 4:
            return w_up.at[:, lanes(k * tall, tall)]
        return w_down.at[pl.ds(pl.multiple_of(k * tall, tall), tall), :]

    def place(kind, plane, k):
        owner = plane * CAST + k
        start = pl.multiple_of(owner * depth, depth)
        if kind < 3:
            return proj.at[pl.ds(start, depth), pl.ds(kind * wide, wide)]
        if kind == 3:
            return mix.at[:, lanes(owner * depth, depth)]
        if kind == 4:
            return up.at[pl.ds(start, depth), :]
        return down.at[k, :, lanes(plane * depth, depth)]

    def swap(kind, i):
        k = peer(i)
        return remote(
            block(kind, k),
            place(kind, g, j),
            swap_send.at[kind, i],
            swap_recv.at[kind, j],
            at(g, k, t),
        )

    def swap_local(kind):
        return pltpu.make_async_copy(block(kind, j), place(kind, g, j), swap_recv.at[kind, j])

    def start_swap(kind):
        for i in range(1, CAST):
            swap(kind, i).start()
        swap_local(kind).start()

    def wait_swap(kind, k):
        pltpu.make_async_copy(
            place(kind, g, k), place(kind, g, k), swap_recv.at[kind, k]
        ).wait()

    chunks = [(kind, None) for kind in range(4)]
    chunks += [(4, q) for q in range(CAST)] + [(5, q) for q in range(CAST)]

    def slab(w, plane):
        kind, q = chunks[w]
        if q is not None:
            return place(kind, plane, q)
        start = pl.multiple_of(plane * CAST * depth, CAST * depth)
        if kind < 3:
            return proj.at[pl.ds(start, CAST * depth), pl.ds(kind * wide, wide)]
        return mix.at[:, lanes(plane * CAST * depth, CAST * depth)]

    def hop(w, plane, up_way):
        return remote(
            slab(w, plane),
            slab(w, plane),
            chain_send.at[w, plane, 1 if up_way else 0],
            chain_recv.at[w, plane],
            at(g + 1 if up_way else g - 1, j, t),
        )

    def pump(step):
        for dist in range(planes):
            w = step - dist
            if w < 0 or w >= len(chunks):
                continue
            if dist == 0:
                kind, q = chunks[w]
                for k in range(CAST) if q is None else (q,):
                    wait_swap(kind, k)

                @pl.when(g < planes - 1)
                def _():
                    hop(w, g, True).start()

                @pl.when(g > 0)
                def _():
                    hop(w, g, False).start()

            else:

                @pl.when(g - dist >= 0)
                def _():
                    source = g - dist
                    pltpu.make_async_copy(
                        slab(w, source), slab(w, source), chain_recv.at[w, source]
                    ).wait()

                    @pl.when(g < planes - 1)
                    def _():
                        hop(w, source, True).start()

                @pl.when(g + dist < planes)
                def _():
                    source = g + dist
                    pltpu.make_async_copy(
                        slab(w, source), slab(w, source), chain_recv.at[w, source]
                    ).wait()

                    @pl.when(g > 0)
                    def _():
                        hop(w, source, False).start()

    def drain():
        for kind in range(6):
            for i in range(1, CAST):
                swap(kind, i).wait_send()
        for w in range(len(chunks)):
            for plane in range(planes):

                @pl.when(jnp.logical_and(g >= plane, g < planes - 1))
                def _():
                    hop(w, plane, True).wait_send()

                @pl.when(jnp.logical_and(g <= plane, g > 0))
                def _():
                    hop(w, plane, False).wait_send()

    def spread(source, i, send, recv):
        return remote(
            source, gathered.at[j, pl.ds(mine, half)], send.at[i], recv.at[i], at(g, peer(i), t)
        )

    def landed(i):
        return gathered.at[lax.rem(j + CAST - i, CAST), pl.ds(mine, half)]

    def relay(i, send, recv):
        return remote(landed(i), landed(i), send.at[i], recv.at[i], partner)

    def relayed(i, recv):
        ref = gathered.at[lax.rem(j + CAST - i, CAST), pl.ds(other, half)]
        return pltpu.make_async_copy(ref, ref, recv.at[i])

    def arrived(i, recv):
        return pltpu.make_async_copy(landed(i), landed(i), recv.at[i])

    def norm(x, gain):
        floats = x.astype(jnp.float32)
        scale = lax.rsqrt(jnp.mean(floats * floats, axis=-1, keepdims=True) + 1e-06)
        return (floats * scale * gain).astype(jnp.bfloat16)

    own = tokens.at[pl.ds(mine, half)]
    for kind in range(4):
        start_swap(kind)
    for i in range(1, CAST):
        spread(own, i, tok_send, tok_recv).start()
    for kind in (4, 5):
        start_swap(kind)
    keep = pltpu.make_async_copy(tokens, gathered.at[j], tok_recv.at[0])
    keep.start()

    for step in range(3):
        pump(step)
    for i in range(1, CAST):
        arrived(i, tok_recv).wait()
        relay(i, fwd_send, fwd_recv).start()
    pump(3)
    for i in range(1, CAST):
        spread(own, i, tok_send, tok_recv).wait_send()
        relay(i, fwd_send, fwd_recv).wait_send()
        relayed(i, fwd_recv).wait()
    keep.wait()
    for step in range(4, 4 + planes - 1):
        pump(step)
    done = 4 + planes - 1

    channel = lanes((t * CAST + j) * wide, wide)
    dims = (((1,), (0,)), ((), ()))

    def dot(a, b):
        return lax.dot_general(a, b, dims, preferred_element_type=jnp.float32)

    def mixer(s):
        @pl.loop(0, rows // STRIP)
        def _(r):
            at_rows = pl.ds(pl.multiple_of(r * STRIP, STRIP), STRIP)
            normed[at_rows, :] = norm(gathered[s, at_rows, :], gain_one[...])

        x = normed[...]
        outer = dot(x, proj[:, 0:wide]).astype(jnp.bfloat16).astype(jnp.float32)
        carrier = dot(x, proj[:, wide : 2 * wide]).astype(jnp.bfloat16).astype(jnp.float32)
        values = dot(x, proj[:, 2 * wide : 3 * wide]).astype(jnp.bfloat16).astype(jnp.float32)
        inner = carrier * values
        count = taps.shape[0]
        position = lax.broadcasted_iota(jnp.int32, inner.shape, 0)
        conv = taps[count - 1 : count, channel] * inner
        for back in range(1, count):
            moved = jnp.where(position >= back, pltpu.roll(inner, back, 0), 0.0)
            conv = conv + taps[count - 1 - back : count - back, channel] * moved
        mixed = (outer * conv).astype(jnp.bfloat16)
        for n in range(0, width, 512):
            part[s, :, n : n + 512] = dot(mixed, mix[:, n : n + 512]).astype(jnp.bfloat16)

    def feed_up(s):
        for n in range(0, tall, 256):
            lifted = jnp.maximum(dot(gathered[s], up[:, n : n + 256]), 0.0)
            hidden[s, :, n : n + 256] = (lifted * lifted).astype(jnp.bfloat16)

    cut = width // CAST

    def part_of(ref, q):
        return ref.at[:, :, pl.ds(q * cut, cut)]

    def feed_down(q):
        @pl.loop(0, CAST)
        def _(s):
            for n in range(0, cut, 256):
                part[s, :, q * cut + n : q * cut + n + 256] = dot(
                    hidden[s], down[q, :, n : n + 256]
                ).astype(jnp.bfloat16)

    def pair_set(q):
        return remote(
            part.at[:, pl.ds(other, half), pl.ds(q * cut, cut)],
            part_of(pair_two, q),
            set_send.at[q, 0],
            set_recv.at[q, 0],
            partner,
        )

    def cross_set(q, i):
        return remote(
            pair_two.at[peer(i), :, pl.ds(q * cut, cut)],
            cross_two.at[i - 1, :, pl.ds(q * cut, cut)],
            set_send.at[q, i],
            set_recv.at[q, i],
            at(g, peer(i), t),
        )

    def sum_set(q):
        pair_set(q).wait_recv()
        at_set = pl.ds(q * cut, cut)
        for i in order:
            s = peer(i)

            @pl.loop(0, half // STRIP)
            def _(r):
                a = part[s, strip(r, mine), at_set].astype(jnp.float32)
                b = pair_two[s, strip(r), at_set].astype(jnp.float32)
                pair_two[s, strip(r), at_set] = (a + b).astype(jnp.bfloat16)

            if i:
                cross_set(q, i).start()

    def finish_set(q):
        for i in range(1, CAST):
            cross_set(q, i).wait_recv()

        @pl.loop(0, half // STRIP)
        def _(r):
            for plane in range(planes):
                source = pl.ds(q * cut + plane * depth, depth)
                target = pl.ds((plane * CAST + q) * depth, depth)
                value = pair_two[j, strip(r), source].astype(jnp.float32)
                for i in range(CAST - 1):
                    value = value + cross_two[i, strip(r), source].astype(jnp.float32)
                value = value + resid[strip(r), target].astype(jnp.float32)
                out[strip(r, mine), target] = value.astype(jnp.bfloat16)

    def pair(turn, i, buffer):
        s = peer(i)
        return remote(
            part.at[s, pl.ds(other, half)],
            buffer.at[s],
            pair_send.at[turn, i],
            pair_recv.at[turn, i],
            partner,
        )

    def pair_wait(turn, i, buffer):
        s = peer(i)
        pltpu.make_async_copy(buffer.at[s], buffer.at[s], pair_recv.at[turn, i]).wait()

    def cross(turn, i, buffer, target):
        return remote(
            buffer.at[peer(i)],
            target.at[i - 1],
            cross_send.at[turn, i],
            cross_recv.at[turn, i],
            at(g, peer(i), t),
        )

    def cross_wait(turn, i, target):
        ref = target.at[i - 1]
        pltpu.make_async_copy(ref, ref, cross_recv.at[turn, i]).wait()

    def strip(r, start=0):
        return pl.ds(pl.multiple_of(start + r * STRIP, STRIP), STRIP)

    def add_pair(i, buffer):
        s = peer(i)

        @pl.loop(0, half // STRIP)
        def _(r):
            a = part[s, strip(r, mine), :].astype(jnp.float32)
            buffer[s, strip(r), :] = (a + buffer[s, strip(r), :].astype(jnp.float32)).astype(
                jnp.bfloat16
            )

    def add_cross(r, buffer, target):
        value = buffer[j, strip(r), :].astype(jnp.float32)
        for i in range(CAST - 1):
            value = value + target[i, strip(r), :].astype(jnp.float32)
        return value

    order = list(range(1, CAST)) + [0]
    for i in order:
        mixer(peer(i))
        pair(0, i, pair_one).start()
        if i == 2:
            pump(done)
    pump(done + 1)
    for i in order:
        pair_wait(0, i, pair_one)
        add_pair(i, pair_one)
        if i:
            cross(0, i, pair_one, cross_one).start()
    pump(done + 2)
    for i in range(1, CAST):
        cross_wait(0, i, cross_one)

    @pl.loop(0, half // STRIP)
    def _(r):
        total_mix = add_cross(r, pair_one, cross_one)
        row = tokens[strip(r, mine), :].astype(jnp.float32) + total_mix
        row = row.astype(jnp.bfloat16)
        resid[strip(r), :] = row
        gathered[j, strip(r, mine), :] = norm(row, gain_two[...])

    fresh = gathered.at[j, pl.ds(mine, half)]
    for i in range(1, CAST):
        spread(fresh, i, sec_send, sec_recv).start()
    relay(0, secf_send, secf_recv).start()
    for i in order:
        pair(0, i, pair_one).wait_send()
        if i:
            cross(0, i, pair_one, cross_one).wait_send()
    pump(done + 3)
    for i in range(1, CAST):
        arrived(i, sec_recv).wait()
        relay(i, secf_send, secf_recv).start()
    for i in order:
        relayed(i, secf_recv).wait()
    for i in order:
        feed_up(peer(i))
    for q in range(CAST):
        pump(done + 4 + q)
        feed_down(q)
        pair_set(q).start()
        sum_set(q)
    for q in range(CAST):
        finish_set(q)

    final = remote(
        out.at[pl.ds(mine, half)],
        out.at[pl.ds(mine, half)],
        last_send.at[0],
        last_recv.at[0],
        partner,
    )
    final.start()
    drain()
    for i in range(1, CAST):
        spread(fresh, i, sec_send, sec_recv).wait_send()
    for i in order:
        relay(i, secf_send, secf_recv).wait_send()
    for q in range(CAST):
        pair_set(q).wait_send()
        for i in range(1, CAST):
            cross_set(q, i).wait_send()
    final.wait()


def fused(
    tokens,
    mixer_norm_gain,
    outer_gate_weight,
    inner_gate_weight,
    value_projection_weight,
    filter_taps_weight,
    mixer_output_weight,
    feedforward_norm_gain,
    up_projection_weight,
    down_projection_weight,
):
    rows, width = tokens.shape
    half = rows // 2
    planes = width // (outer_gate_weight.shape[0] * CAST)
    wide = outer_gate_weight.shape[1] // CAST
    tall = up_projection_weight.shape[1] // CAST
    dma = pltpu.SemaphoreType.DMA
    chunk_count = 4 + 2 * CAST
    bf16 = jnp.bfloat16
    return pl.pallas_call(
        functools.partial(fused_kernel, planes),
        out_shape=jax.ShapeDtypeStruct((rows, width), bf16),
        in_specs=[pl.BlockSpec(memory_space=pltpu.VMEM)] * 10,
        out_specs=pl.BlockSpec(memory_space=pltpu.VMEM),
        scratch_shapes=[
            pltpu.VMEM((width, 3 * wide), bf16),
            pltpu.VMEM((wide, width), bf16),
            pltpu.VMEM((width, tall), bf16),
            pltpu.VMEM((CAST, tall, width // CAST), bf16),
            pltpu.VMEM((CAST, rows, width), bf16),
            pltpu.VMEM((rows, width), bf16),
            pltpu.VMEM((CAST, rows, tall), bf16),
            pltpu.VMEM((CAST, rows, width), bf16),
            pltpu.VMEM((CAST, half, width), bf16),
            pltpu.VMEM((CAST, half, width), bf16),
            pltpu.VMEM((CAST - 1, half, width), bf16),
            pltpu.VMEM((CAST - 1, half, width), bf16),
            pltpu.VMEM((half, width), bf16),
            dma((6, CAST)),
            dma((6, CAST)),
            dma((chunk_count, planes, 2)),
            dma((chunk_count, planes)),
            dma((CAST,)),
            dma((CAST,)),
            dma((CAST,)),
            dma((CAST,)),
            dma((CAST,)),
            dma((CAST,)),
            dma((CAST,)),
            dma((CAST,)),
            dma((1, CAST)),
            dma((1, CAST)),
            dma((1, CAST)),
            dma((1, CAST)),
            dma((CAST, CAST)),
            dma((CAST, CAST)),
            dma((1,)),
            dma((1,)),
        ],
        compiler_params=pltpu.CompilerParams(
            collective_id=1, has_side_effects=True, vmem_limit_bytes=63 * 1024 * 1024
        ),
        name="fused_layer",
    )(
        tokens,
        mixer_norm_gain.reshape(1, -1),
        outer_gate_weight,
        inner_gate_weight,
        value_projection_weight,
        filter_taps_weight,
        mixer_output_weight,
        feedforward_norm_gain.reshape(1, -1),
        up_projection_weight,
        down_projection_weight,
    )


def layer(*args):
    tokens, outer, up = args[0], args[2], args[8]
    depth = outer.shape[0]
    fits = (
        lax.axis_size("tp") == 2
        and lax.axis_size("fs") % CAST == 0
        and depth % 128 == 0
        and outer.shape[1] % (CAST * 128) == 0
        and up.shape[1] % (CAST * 256) == 0
        and tokens.shape[0] % (2 * STRIP) == 0
        and tokens.shape[1] % 512 == 0
    )
    return fused(*args) if fits else on_device(*args)


def solution(mesh):
    return jax.shard_map(
        layer,
        mesh=mesh,
        in_specs=(
            P("fs", None),
            P(),
            P("fs", "tp"),
            P("fs", "tp"),
            P("fs", "tp"),
            P(),
            P("tp", "fs"),
            P(),
            P("fs", "tp"),
            P("tp", "fs"),
        ),
        out_specs=P("fs", None),
        check_vma=False,
    )
```

```python
import functools

import jax
import jax.numpy as jnp
from jax import lax
from jax.experimental import pallas as pl
from jax.experimental.pallas import tpu as pltpu
from jax.sharding import PartitionSpec as P


def rms_norm(rows, gain):
    floats = rows.astype(jnp.float32)
    scale = lax.rsqrt(jnp.mean(floats * floats, axis=-1, keepdims=True) + 1e-06)
    return (floats * scale * gain).astype(jnp.bfloat16)


def causal_mix(inner_product_rows, taps):
    length = inner_product_rows.shape[0]
    width = taps.shape[0]
    padded = jnp.pad(inner_product_rows, ((width - 1, 0), (0, 0)))
    total = jnp.zeros_like(inner_product_rows)
    for offset in range(width):
        total = total + taps[offset] * padded[offset : offset + length]
    return total


def settle(partial_value):
    rounded = lax.optimization_barrier(partial_value.astype(jnp.bfloat16))
    return rounded.astype(jnp.float32)


def on_device(
    tokens,
    mixer_norm_gain,
    outer_gate_weight,
    inner_gate_weight,
    value_projection_weight,
    filter_taps_weight,
    mixer_output_weight,
    feedforward_norm_gain,
    up_projection_weight,
    down_projection_weight,
):
    index = lax.axis_index("tp")
    local_width = outer_gate_weight.shape[1]
    first_normed_rows = rms_norm(tokens, mixer_norm_gain)
    pieces = (
        lax.all_gather(outer_gate_weight, "fs", axis=0, tiled=True),
        lax.all_gather(inner_gate_weight, "fs", axis=0, tiled=True),
        lax.all_gather(value_projection_weight, "fs", axis=0, tiled=True),
    )
    columns = first_normed_rows
    outer_gate_rows, inner_gate_rows, value_rows = tuple(
        (jnp.dot(columns, piece, preferred_element_type=jnp.float32) for piece in pieces)
    )
    outer_gate_rows = outer_gate_rows.astype(jnp.bfloat16)
    inner_gate_rows = inner_gate_rows.astype(jnp.bfloat16)
    value_rows = value_rows.astype(jnp.bfloat16)
    taps = lax.dynamic_slice_in_dim(filter_taps_weight, index * local_width, local_width, 1)
    inner_product_rows = inner_gate_rows.astype(jnp.float32) * value_rows.astype(jnp.float32)
    mixed = (outer_gate_rows.astype(jnp.float32) * causal_mix(inner_product_rows, taps)).astype(
        jnp.bfloat16
    )
    partial_value = settle(
        jnp.dot(
            mixed,
            lax.all_gather(mixer_output_weight, "fs", axis=1, tiled=True),
            preferred_element_type=jnp.float32,
        )
    )
    total = lax.psum(partial_value.astype(jnp.bfloat16), "tp").astype(jnp.float32)
    resid = (tokens.astype(jnp.float32) + total).astype(jnp.bfloat16)
    second = rms_norm(resid, feedforward_norm_gain)
    columns = second
    lifted = jnp.maximum(
        jnp.dot(
            columns,
            lax.all_gather(up_projection_weight, "fs", axis=0, tiled=True),
            preferred_element_type=jnp.float32,
        ),
        0.0,
    )
    hidden = (lifted * lifted).astype(jnp.bfloat16)
    down = jnp.dot(
        hidden,
        lax.all_gather(down_projection_weight, "fs", axis=1, tiled=True),
        preferred_element_type=jnp.float32,
    )
    total_down = lax.psum(settle(down).astype(jnp.bfloat16), "tp").astype(jnp.float32)
    return (resid.astype(jnp.float32) + total_down).astype(jnp.bfloat16)


MESH = pl.DeviceIdType.MESH
CAST = 4
STRIP = 64


def fused_kernel(
    planes,
    tokens,
    gain_one,
    w_outer,
    w_inner,
    w_value,
    taps,
    w_mix,
    gain_two,
    w_up,
    w_down,
    out,
    proj,
    mix,
    up,
    down,
    gathered,
    normed,
    hidden,
    part,
    pair_one,
    pair_two,
    cross_one,
    cross_two,
    resid,
    swap_send,
    swap_recv,
    chain_send,
    chain_recv,
    tok_send,
    tok_recv,
    fwd_send,
    fwd_recv,
    sec_send,
    sec_recv,
    secf_send,
    secf_recv,
    pair_send,
    pair_recv,
    cross_send,
    cross_recv,
    set_send,
    set_recv,
    last_send,
    last_recv,
):
    f = lax.axis_index("fs")
    t = lax.axis_index("tp")
    g = f // CAST
    j = lax.rem(f, CAST)
    rows = tokens.shape[0]
    half = rows // 2
    depth = w_outer.shape[0]
    wide = w_outer.shape[1] // CAST
    tall = w_up.shape[1] // CAST
    width = tokens.shape[1]
    mine = pl.multiple_of(t * half, half)
    other = pl.multiple_of((1 - t) * half, half)

    def peer(i):
        return lax.rem(j + i, CAST)

    def at(plane, k, core):
        return {"fs": plane * CAST + k, "tp": core}

    partner = at(g, j, 1 - t)

    def remote(src, dst, send, recv, device):
        return pltpu.make_async_remote_copy(
            src_ref=src,
            dst_ref=dst,
            send_sem=send,
            recv_sem=recv,
            device_id=device,
            device_id_type=MESH,
        )

    barrier = pltpu.get_barrier_semaphore()
    for i in range(1, CAST):
        pl.semaphore_signal(barrier, inc=1, device_id=at(g, peer(i), t), device_id_type=MESH)
    pl.semaphore_signal(barrier, inc=1, device_id=partner, device_id_type=MESH)

    @pl.when(g > 0)
    def _():
        pl.semaphore_signal(barrier, inc=1, device_id=at(g - 1, j, t), device_id_type=MESH)

    @pl.when(g < planes - 1)
    def _():
        pl.semaphore_signal(barrier, inc=1, device_id=at(g + 1, j, t), device_id_type=MESH)

    ends = jnp.minimum(g, 1) + jnp.minimum(planes - 1 - g, 1)
    pl.semaphore_wait(barrier, CAST + ends)

    def lanes(start, size):
        return pl.ds(pl.multiple_of(start, 128), size)

    shards = (w_outer, w_inner, w_value, w_mix, w_up, w_down)

    def block(kind, k):
        if kind < 3:
            return shards[kind].at[:, lanes(k * wide, wide)]
        if kind == 3:
            return w_mix.at[pl.ds(pl.multiple_of(k * wide, wide), wide), :]
        if kind == 4:
            return w_up.at[:, lanes(k * tall, tall)]
        return w_down.at[pl.ds(pl.multiple_of(k * tall, tall), tall), :]

    def place(kind, plane, k):
        owner = plane * CAST + k
        start = pl.multiple_of(owner * depth, depth)
        if kind < 3:
            return proj.at[pl.ds(start, depth), pl.ds(kind * wide, wide)]
        if kind == 3:
            return mix.at[:, lanes(owner * depth, depth)]
        if kind == 4:
            return up.at[pl.ds(start, depth), :]
        return down.at[k, :, lanes(plane * depth, depth)]

    def swap(kind, i):
        k = peer(i)
        return remote(
            block(kind, k),
            place(kind, g, j),
            swap_send.at[kind, i],
            swap_recv.at[kind, j],
            at(g, k, t),
        )

    def swap_local(kind):
        return pltpu.make_async_copy(block(kind, j), place(kind, g, j), swap_recv.at[kind, j])

    def start_swap(kind):
        for i in range(1, CAST):
            swap(kind, i).start()
        swap_local(kind).start()

    def wait_swap(kind, k):
        pltpu.make_async_copy(
            place(kind, g, k), place(kind, g, k), swap_recv.at[kind, k]
        ).wait()

    chunks = [((0, 1, 2), None), ((3,), None)]
    chunks += [((4,), q) for q in range(CAST)] + [((5,), q) for q in range(CAST)]
    lead = 2

    def slab(w, plane):
        kinds, q = chunks[w]
        if q is not None:
            return place(kinds[0], plane, q)
        start = pl.multiple_of(plane * CAST * depth, CAST * depth)
        if len(kinds) > 1:
            return proj.at[pl.ds(start, CAST * depth), :]
        return mix.at[:, lanes(plane * CAST * depth, CAST * depth)]

    def hop(w, plane, up_way):
        return remote(
            slab(w, plane),
            slab(w, plane),
            chain_send.at[w, plane, 1 if up_way else 0],
            chain_recv.at[w, plane],
            at(g + 1 if up_way else g - 1, j, t),
        )

    def pump(step):
        for dist in range(planes):
            w = step - dist
            if w < 0 or w >= len(chunks):
                continue
            if dist == 0:
                kinds, q = chunks[w]
                for k in range(CAST) if q is None else (q,):
                    for kind in kinds:
                        wait_swap(kind, k)

                @pl.when(g < planes - 1)
                def _():
                    hop(w, g, True).start()

                @pl.when(g > 0)
                def _():
                    hop(w, g, False).start()

            else:

                @pl.when(g - dist >= 0)
                def _():
                    source = g - dist
                    pltpu.make_async_copy(
                        slab(w, source), slab(w, source), chain_recv.at[w, source]
                    ).wait()

                    @pl.when(g < planes - 1)
                    def _():
                        hop(w, source, True).start()

                @pl.when(g + dist < planes)
                def _():
                    source = g + dist
                    pltpu.make_async_copy(
                        slab(w, source), slab(w, source), chain_recv.at[w, source]
                    ).wait()

                    @pl.when(g > 0)
                    def _():
                        hop(w, source, False).start()

    def drain():
        for kind in range(6):
            for i in range(1, CAST):
                swap(kind, i).wait_send()
        for w in range(len(chunks)):
            for plane in range(planes):

                @pl.when(jnp.logical_and(g >= plane, g < planes - 1))
                def _():
                    hop(w, plane, True).wait_send()

                @pl.when(jnp.logical_and(g <= plane, g > 0))
                def _():
                    hop(w, plane, False).wait_send()

    def spread(source, i, send, recv):
        return remote(
            source, gathered.at[j, pl.ds(mine, half)], send.at[i], recv.at[i], at(g, peer(i), t)
        )

    def landed(i):
        return gathered.at[lax.rem(j + CAST - i, CAST), pl.ds(mine, half)]

    def relay(i, send, recv):
        return remote(landed(i), landed(i), send.at[i], recv.at[i], partner)

    def relayed(i, recv):
        ref = gathered.at[lax.rem(j + CAST - i, CAST), pl.ds(other, half)]
        return pltpu.make_async_copy(ref, ref, recv.at[i])

    def arrived(i, recv):
        return pltpu.make_async_copy(landed(i), landed(i), recv.at[i])

    def norm(x, gain):
        floats = x.astype(jnp.float32)
        scale = lax.rsqrt(jnp.mean(floats * floats, axis=-1, keepdims=True) + 1e-06)
        return (floats * scale * gain).astype(jnp.bfloat16)

    own = tokens.at[pl.ds(mine, half)]
    for kind in range(4):
        start_swap(kind)
    for i in range(1, CAST):
        spread(own, i, tok_send, tok_recv).start()
    for kind in (4, 5):
        start_swap(kind)
    keep = pltpu.make_async_copy(tokens, gathered.at[j], tok_recv.at[0])
    keep.start()

    for step in range(3):
        pump(step)
    for i in range(1, CAST):
        arrived(i, tok_recv).wait()
        relay(i, fwd_send, fwd_recv).start()
    pump(3)
    for i in range(1, CAST):
        spread(own, i, tok_send, tok_recv).wait_send()
        relay(i, fwd_send, fwd_recv).wait_send()
        relayed(i, fwd_recv).wait()
    keep.wait()
    for step in range(4, lead + planes - 1):
        pump(step)
    done = max(lead + planes - 1, 4)

    channel = lanes((t * CAST + j) * wide, wide)
    dims = (((1,), (0,)), ((), ()))

    def dot(a, b):
        return lax.dot_general(a, b, dims, preferred_element_type=jnp.float32)

    def mixer(s):
        @pl.loop(0, rows // STRIP)
        def _(r):
            at_rows = pl.ds(pl.multiple_of(r * STRIP, STRIP), STRIP)
            normed[at_rows, :] = norm(gathered[s, at_rows, :], gain_one[...])

        x = normed[...]
        outer = dot(x, proj[:, 0:wide]).astype(jnp.bfloat16).astype(jnp.float32)
        carrier = dot(x, proj[:, wide : 2 * wide]).astype(jnp.bfloat16).astype(jnp.float32)
        values = dot(x, proj[:, 2 * wide : 3 * wide]).astype(jnp.bfloat16).astype(jnp.float32)
        inner = carrier * values
        count = taps.shape[0]
        position = lax.broadcasted_iota(jnp.int32, inner.shape, 0)
        conv = taps[count - 1 : count, channel] * inner
        for back in range(1, count):
            moved = jnp.where(position >= back, pltpu.roll(inner, back, 0), 0.0)
            conv = conv + taps[count - 1 - back : count - back, channel] * moved
        mixed = (outer * conv).astype(jnp.bfloat16)
        for n in range(0, width, 512):
            part[s, :, n : n + 512] = dot(mixed, mix[:, n : n + 512]).astype(jnp.bfloat16)

    def feed_up(s):
        for n in range(0, tall, 256):
            lifted = jnp.maximum(dot(gathered[s], up[:, n : n + 256]), 0.0)
            hidden[s, :, n : n + 256] = (lifted * lifted).astype(jnp.bfloat16)

    cut = width // CAST

    def part_of(ref, q):
        return ref.at[:, :, pl.ds(q * cut, cut)]

    def feed_down(q):
        @pl.loop(0, CAST)
        def _(s):
            for n in range(0, cut, 256):
                part[s, :, q * cut + n : q * cut + n + 256] = dot(
                    hidden[s], down[q, :, n : n + 256]
                ).astype(jnp.bfloat16)

    def pair_set(q):
        return remote(
            part.at[:, pl.ds(other, half), pl.ds(q * cut, cut)],
            part_of(pair_two, q),
            set_send.at[q, 0],
            set_recv.at[q, 0],
            partner,
        )

    def cross_set(q, i):
        return remote(
            pair_two.at[peer(i), :, pl.ds(q * cut, cut)],
            cross_two.at[i - 1, :, pl.ds(q * cut, cut)],
            set_send.at[q, i],
            set_recv.at[q, i],
            at(g, peer(i), t),
        )

    def sum_set(q):
        pair_set(q).wait_recv()
        at_set = pl.ds(q * cut, cut)
        for i in order:
            s = peer(i)

            @pl.loop(0, half // STRIP)
            def _(r):
                a = part[s, strip(r, mine), at_set].astype(jnp.float32)
                b = pair_two[s, strip(r), at_set].astype(jnp.float32)
                pair_two[s, strip(r), at_set] = (a + b).astype(jnp.bfloat16)

            if i:
                cross_set(q, i).start()

    def finish_set(q):
        for i in range(1, CAST):
            cross_set(q, i).wait_recv()

        @pl.loop(0, half // STRIP)
        def _(r):
            for plane in range(planes):
                source = pl.ds(q * cut + plane * depth, depth)
                target = pl.ds((plane * CAST + q) * depth, depth)
                value = pair_two[j, strip(r), source].astype(jnp.float32)
                for i in range(CAST - 1):
                    value = value + cross_two[i, strip(r), source].astype(jnp.float32)
                value = value + resid[strip(r), target].astype(jnp.float32)
                out[strip(r, mine), target] = value.astype(jnp.bfloat16)

    def pair(turn, i, buffer):
        s = peer(i)
        return remote(
            part.at[s, pl.ds(other, half)],
            buffer.at[s],
            pair_send.at[turn, i],
            pair_recv.at[turn, i],
            partner,
        )

    def pair_wait(turn, i, buffer):
        s = peer(i)
        pltpu.make_async_copy(buffer.at[s], buffer.at[s], pair_recv.at[turn, i]).wait()

    def cross(turn, i, buffer, target):
        return remote(
            buffer.at[peer(i)],
            target.at[i - 1],
            cross_send.at[turn, i],
            cross_recv.at[turn, i],
            at(g, peer(i), t),
        )

    def cross_wait(turn, i, target):
        ref = target.at[i - 1]
        pltpu.make_async_copy(ref, ref, cross_recv.at[turn, i]).wait()

    def strip(r, start=0):
        return pl.ds(pl.multiple_of(start + r * STRIP, STRIP), STRIP)

    def add_pair(i, buffer):
        s = peer(i)

        @pl.loop(0, half // STRIP)
        def _(r):
            a = part[s, strip(r, mine), :].astype(jnp.float32)
            buffer[s, strip(r), :] = (a + buffer[s, strip(r), :].astype(jnp.float32)).astype(
                jnp.bfloat16
            )

    def add_cross(r, buffer, target):
        value = buffer[j, strip(r), :].astype(jnp.float32)
        for i in range(CAST - 1):
            value = value + target[i, strip(r), :].astype(jnp.float32)
        return value

    order = list(range(1, CAST)) + [0]
    for i in order:
        mixer(peer(i))
        pair(0, i, pair_one).start()
        if i == 2:
            pump(done)
    pump(done + 1)
    for i in order:
        pair_wait(0, i, pair_one)
        add_pair(i, pair_one)
        if i:
            cross(0, i, pair_one, cross_one).start()
    pump(done + 2)
    for i in range(1, CAST):
        cross_wait(0, i, cross_one)

    @pl.loop(0, half // STRIP)
    def _(r):
        total_mix = add_cross(r, pair_one, cross_one)
        row = tokens[strip(r, mine), :].astype(jnp.float32) + total_mix
        row = row.astype(jnp.bfloat16)
        resid[strip(r), :] = row
        gathered[j, strip(r, mine), :] = norm(row, gain_two[...])

    fresh = gathered.at[j, pl.ds(mine, half)]
    for i in range(1, CAST):
        spread(fresh, i, sec_send, sec_recv).start()
    relay(0, secf_send, secf_recv).start()
    for i in order:
        pair(0, i, pair_one).wait_send()
        if i:
            cross(0, i, pair_one, cross_one).wait_send()
    pump(done + 3)
    for i in range(1, CAST):
        arrived(i, sec_recv).wait()
        relay(i, secf_send, secf_recv).start()
    for i in order:
        relayed(i, secf_recv).wait()
    for i in order:
        feed_up(peer(i))
    for q in range(CAST):
        pump(done + 4 + q)
        feed_down(q)
        pair_set(q).start()
        sum_set(q)
    for q in range(CAST):
        finish_set(q)

    final = remote(
        out.at[pl.ds(mine, half)],
        out.at[pl.ds(mine, half)],
        last_send.at[0],
        last_recv.at[0],
        partner,
    )
    final.start()
    drain()
    for i in range(1, CAST):
        spread(fresh, i, sec_send, sec_recv).wait_send()
    for i in order:
        relay(i, secf_send, secf_recv).wait_send()
    for q in range(CAST):
        pair_set(q).wait_send()
        for i in range(1, CAST):
            cross_set(q, i).wait_send()
    final.wait()


def fused(
    tokens,
    mixer_norm_gain,
    outer_gate_weight,
    inner_gate_weight,
    value_projection_weight,
    filter_taps_weight,
    mixer_output_weight,
    feedforward_norm_gain,
    up_projection_weight,
    down_projection_weight,
):
    rows, width = tokens.shape
    half = rows // 2
    planes = width // (outer_gate_weight.shape[0] * CAST)
    wide = outer_gate_weight.shape[1] // CAST
    tall = up_projection_weight.shape[1] // CAST
    dma = pltpu.SemaphoreType.DMA
    chunk_count = 2 + 2 * CAST
    bf16 = jnp.bfloat16
    return pl.pallas_call(
        functools.partial(fused_kernel, planes),
        out_shape=jax.ShapeDtypeStruct((rows, width), bf16),
        in_specs=[pl.BlockSpec(memory_space=pltpu.VMEM)] * 10,
        out_specs=pl.BlockSpec(memory_space=pltpu.VMEM),
        scratch_shapes=[
            pltpu.VMEM((width, 3 * wide), bf16),
            pltpu.VMEM((wide, width), bf16),
            pltpu.VMEM((width, tall), bf16),
            pltpu.VMEM((CAST, tall, width // CAST), bf16),
            pltpu.VMEM((CAST, rows, width), bf16),
            pltpu.VMEM((rows, width), bf16),
            pltpu.VMEM((CAST, rows, tall), bf16),
            pltpu.VMEM((CAST, rows, width), bf16),
            pltpu.VMEM((CAST, half, width), bf16),
            pltpu.VMEM((CAST, half, width), bf16),
            pltpu.VMEM((CAST - 1, half, width), bf16),
            pltpu.VMEM((CAST - 1, half, width), bf16),
            pltpu.VMEM((half, width), bf16),
            dma((6, CAST)),
            dma((6, CAST)),
            dma((chunk_count, planes, 2)),
            dma((chunk_count, planes)),
            dma((CAST,)),
            dma((CAST,)),
            dma((CAST,)),
            dma((CAST,)),
            dma((CAST,)),
            dma((CAST,)),
            dma((CAST,)),
            dma((CAST,)),
            dma((1, CAST)),
            dma((1, CAST)),
            dma((1, CAST)),
            dma((1, CAST)),
            dma((CAST, CAST)),
            dma((CAST, CAST)),
            dma((1,)),
            dma((1,)),
        ],
        compiler_params=pltpu.CompilerParams(
            collective_id=1, has_side_effects=True, vmem_limit_bytes=63 * 1024 * 1024
        ),
        name="fused_layer",
    )(
        tokens,
        mixer_norm_gain.reshape(1, -1),
        outer_gate_weight,
        inner_gate_weight,
        value_projection_weight,
        filter_taps_weight,
        mixer_output_weight,
        feedforward_norm_gain.reshape(1, -1),
        up_projection_weight,
        down_projection_weight,
    )


def layer(*args):
    tokens, outer, up = args[0], args[2], args[8]
    depth = outer.shape[0]
    fits = (
        lax.axis_size("tp") == 2
        and lax.axis_size("fs") % CAST == 0
        and depth % 128 == 0
        and outer.shape[1] % (CAST * 128) == 0
        and up.shape[1] % (CAST * 256) == 0
        and tokens.shape[0] % (2 * STRIP) == 0
        and tokens.shape[1] % 512 == 0
    )
    return fused(*args) if fits else on_device(*args)


def solution(mesh):
    return jax.shard_map(
        layer,
        mesh=mesh,
        in_specs=(
            P("fs", None),
            P(),
            P("fs", "tp"),
            P("fs", "tp"),
            P("fs", "tp"),
            P(),
            P("tp", "fs"),
            P(),
            P("fs", "tp"),
            P("tp", "fs"),
        ),
        out_specs=P("fs", None),
        check_vma=False,
    )
```
